128 devices in a mesh: sp: 16 (over z, y), fs: 4 (over x), tp: 2 (over core).
Axes of the slice: x: 4, y: 4, z: 4, core: 2. Of those that a mesh axis runs over, the one named last changes fastest.
Arguments:
- tokens: bfloat16 [65536, 2048], P(('fs', 'sp', 'tp')), parts along dimension 0, may hold values from -6 to 6
- norm_gain: float32 [2048], replicated, may hold values from 0.1 to 1.9
- w_pool: bfloat16 [2048, 1024], P(None, 'tp'), may hold values from -0.125 to 0.125
- w_query: bfloat16 [2048, 1024], P(None, 'tp'), may hold values from -0.125 to 0.125
- w_key: bfloat16 [2048, 1024], P(None, 'tp'), may hold values from -0.125 to 0.125
- w_value: bfloat16 [2048, 1024], P(None, 'tp'), may hold values from -0.125 to 0.125
- w_gate: bfloat16 [2048, 1024], P(None, 'tp'), may hold values from -0.125 to 0.125
- pool_mix: bfloat16 [4, 256, 256], P('tp'), may hold values from -0.375 to 0.375
- pool_bias: float32 [4, 256], P('tp'), may hold values from -3 to 3
- pool_gain: float32 [1024], P('tp'), may hold values from 0.1 to 1.9
- ret_gain: float32 [1024], P('tp'), may hold values from 0.1 to 1.9
- w_out_pool: bfloat16 [1024, 2048], P('tp'), may hold values from -0.125 to 0.125
- w_out_ret: bfloat16 [1024, 2048], P('tp'), may hold values from -0.125 to 0.125
Outputs:
- mixed: bfloat16 [65536, 2048], P(('fs', 'sp', 'tp')), parts along dimension 0
The draws below stay inside these ranges and needn't reach their ends.
There are 4 independent parts, one for each index of `fs`. The reference program is written for one: setup_inputs(seed, part) draws one part's arguments, and reference() takes and returns one part's arrays. A program takes and returns all parts, laid end to end along the dimension named above; an argument that names none is the same for every part. Nothing has to cross between parts.
All inputs are finite; a program needn't handle non-finite values.
Results may differ from the reference program's by a relative error of at most 0.012.
Values may be sent and summed in bfloat16 or wider, within the bound.
No kernel may reach another device: no remote copies, remote signals or barrier semaphores. Data moves between devices by JAX's collectives and lax.ppermute only.
A program may use at most 128 MiB of HBM per device.

```python
import jax
import jax.numpy as jnp
from jax import lax

D = 2048
GROUP_DIM = 256
POOL_WIDTH = 1024
HEADS = 8
HEAD_DIM = 128
RET_WIDTH = 1024
BLOCK = 128
SEQ = 16384
N_TP = 2


def level_of(own_key, shape, cuts, smallest, high):
    factor_of, own = 1.0, jax.random.fold_in(own_key, 6)
    for dim, shards_of in cuts:
        steps = jnp.exp(jax.random.uniform(jax.random.fold_in(own, dim), (shards_of,), jnp.float32, smallest / len(cuts), high / len(cuts)))
        factor_of = factor_of * jnp.repeat(steps, shape[dim] // shards_of).reshape([-1 if axis == dim else 1 for axis in range(len(shape))])
    return factor_of


def noise(rng, extent, width, bound, cuts=(), kind=jnp.bfloat16):
    level = level_of(rng, extent, cuts, -0.22, 0.18) if cuts else 1.0
    entries = jax.random.normal(rng, extent, jnp.float32) * width * level
    return jnp.minimum(jnp.maximum(entries, -bound), bound).astype(kind)


def setup_inputs(seed: int = 0, part: int = 0) -> dict:
    splits = jax.random.split(jax.random.key(seed), 14)
    part_splits = jax.random.split(jax.random.fold_in(splits[13], part), 14)
    return {
        "tokens": noise(part_splits[0], (SEQ, D), 1.0, 6.0, ((0, 32),)),
        "norm_gain": jnp.clip(1.0 + 0.18 * jax.random.normal(splits[1], (D,), jnp.float32), 0.1, 1.9),
        "w_pool": noise(splits[2], (D, POOL_WIDTH), D ** -0.5, 0.125, ((1, 2),)),
        "w_query": noise(splits[3], (D, RET_WIDTH), D ** -0.5, 0.125, ((1, 2),)),
        "w_key": noise(splits[4], (D, RET_WIDTH), D ** -0.5, 0.125, ((1, 2),)),
        "w_value": noise(splits[5], (D, RET_WIDTH), D ** -0.5, 0.125, ((1, 2),)),
        "w_gate": noise(splits[6], (D, RET_WIDTH), D ** -0.5, 0.125, ((1, 2),)),
        "pool_mix": noise(splits[7], (4, GROUP_DIM, GROUP_DIM), GROUP_DIM ** -0.5, 0.375, ((0, 2),)),
        "pool_bias": noise(splits[8], (4, GROUP_DIM), 0.5, 3.0, ((0, 2),), jnp.float32),
        "pool_gain": jnp.clip(1.0 + 0.18 * jax.random.normal(splits[9], (POOL_WIDTH,), jnp.float32), 0.1, 1.9),
        "ret_gain": jnp.clip(1.0 + 0.18 * jax.random.normal(splits[10], (RET_WIDTH,), jnp.float32), 0.1, 1.9),
        "w_out_pool": noise(splits[11], (POOL_WIDTH, D), (POOL_WIDTH + RET_WIDTH) ** -0.5, 0.125, ((0, 2),)),
        "w_out_ret": noise(splits[12], (RET_WIDTH, D), (POOL_WIDTH + RET_WIDTH) ** -0.5, 0.125, ((0, 2),)),
    }


def rotary(values, positions):
    half = values.shape[-1] // 2
    inverse = 10000.0 ** (-jnp.arange(half, dtype=jnp.float32) / half)
    angles = positions[:, None] * inverse[None, :]
    cosine = jnp.cos(angles)[:, None, :]
    sine = jnp.sin(angles)[:, None, :]
    first = values[..., :half]
    second = values[..., half:]
    return jnp.concatenate([first * cosine - second * sine, second * cosine + first * sine], axis=-1)

def retain(query, key, value, log_decay):
    length = query.shape[0]
    blocks = length // BLOCK
    hp = lax.Precision.HIGHEST

    def split(values):
        return values.reshape(blocks, BLOCK, HEADS, HEAD_DIM).transpose(0, 2, 1, 3)
    steps = jnp.arange(BLOCK, dtype=jnp.float32)
    apart = steps[:, None] - steps[None, :]
    inner = jnp.where(apart[None] >= 0, jnp.exp(log_decay[:, None, None] * jnp.maximum(apart, 0.0)[None]), 0.0)
    query_decay = jnp.exp(log_decay[:, None] * (steps[None, :] + 1.0))
    key_decay = jnp.exp(log_decay[:, None] * (BLOCK - 1.0 - steps[None, :]))
    block_decay = jnp.exp(log_decay * BLOCK)

    def advance(state, pieces):
        qb, kb, vb = pieces
        scores = jnp.einsum('hid,hjd->hij', qb, kb, precision=hp) * inner
        out = jnp.einsum('hij,hje->hie', scores, vb, precision=hp)
        out = out + jnp.einsum('hid,hde->hie', qb, state, precision=hp) * query_decay[:, :, None]
        state = state * block_decay[:, None, None] + jnp.einsum('hjd,hje->hde', kb * key_decay[:, :, None], vb, precision=hp)
        return (state, out)
    start = jnp.zeros((HEADS, HEAD_DIM, HEAD_DIM), jnp.float32)
    state, outs = lax.scan(advance, start, (split(query), split(key), split(value)))
    return outs.transpose(0, 2, 1, 3).reshape(length, HEADS, HEAD_DIM)

def reference(tokens, norm_gain, w_pool, w_query, w_key, w_value, w_gate, pool_mix, pool_bias, pool_gain, ret_gain, w_out_pool, w_out_ret):
    xf = tokens.astype(jnp.float32)
    normed = (xf * lax.rsqrt(lax.optimization_barrier(jnp.mean(xf * xf, axis=-1, keepdims=True)) + 1e-06) * norm_gain).astype(jnp.bfloat16)
    pool_in = jnp.dot(normed, w_pool, preferred_element_type=jnp.float32).astype(jnp.bfloat16)
    query = jnp.dot(normed, w_query, preferred_element_type=jnp.float32).astype(jnp.bfloat16)
    key = jnp.dot(normed, w_key, preferred_element_type=jnp.float32).astype(jnp.bfloat16)
    value = jnp.dot(normed, w_value, preferred_element_type=jnp.float32).astype(jnp.bfloat16)
    gate = jnp.dot(normed, w_gate, preferred_element_type=jnp.float32).astype(jnp.bfloat16)
    positions = jnp.arange(SEQ, dtype=jnp.float32)
    groups = []
    for group in range(4):
        window = 2 ** (group + 1)
        block = pool_in[:, group * GROUP_DIM:(group + 1) * GROUP_DIM].astype(jnp.float32)
        running = jnp.cumsum(block, axis=0)
        padded = jnp.concatenate([jnp.zeros((window, GROUP_DIM), jnp.float32), running], axis=0)
        window_sum = padded[window:] - padded[:SEQ]
        count = jnp.minimum(positions + 1.0, float(window))[:, None]
        diff = (window_sum / count - block).astype(jnp.bfloat16)
        mixed_group = jnp.dot(diff, pool_mix[group], preferred_element_type=jnp.float32) + pool_bias[group][None, :]
        groups.append(mixed_group)
    pool_out = (jnp.concatenate(groups, axis=1) * pool_gain[None, :]).astype(jnp.bfloat16)
    head_ids = jnp.arange(HEADS, dtype=jnp.float32)
    log_decay = -2.0 ** (-5) * (SEQ / 16.0) ** (-2.0 * head_ids / (HEADS - 1))
    qf = rotary(query.astype(jnp.float32).reshape(SEQ, HEADS, HEAD_DIM), positions)
    kf = rotary(key.astype(jnp.float32).reshape(SEQ, HEADS, HEAD_DIM), positions) * HEAD_DIM ** (-0.5)
    vf = value.astype(jnp.float32).reshape(SEQ, HEADS, HEAD_DIM)
    raw = retain(qf, kf, vf, log_decay)
    mean = lax.optimization_barrier(jnp.mean(raw, axis=-1, keepdims=True))
    var = lax.optimization_barrier(jnp.mean(jnp.square(raw - mean), axis=-1, keepdims=True))
    normalized = ((raw - mean) * lax.rsqrt(var + 1e-06)).reshape(SEQ, RET_WIDTH) * ret_gain[None, :]
    ret_out = (jax.nn.silu(gate.astype(jnp.float32)) * normalized).astype(jnp.bfloat16)
    pool_share = POOL_WIDTH // N_TP
    ret_share = RET_WIDTH // N_TP
    total = jnp.zeros((SEQ, D), jnp.float32)
    for index in range(N_TP):
        part_pool = jnp.dot(pool_out[:, index * pool_share:(index + 1) * pool_share], w_out_pool[index * pool_share:(index + 1) * pool_share], preferred_element_type=jnp.float32)
        part_ret = jnp.dot(ret_out[:, index * ret_share:(index + 1) * ret_share], w_out_ret[index * ret_share:(index + 1) * ret_share], preferred_element_type=jnp.float32)
        total = total + (part_pool + part_ret).astype(jnp.bfloat16).astype(jnp.float32)
    return total.astype(jnp.bfloat16)
```

```python
import functools

import jax
import jax.numpy as jnp
import numpy as np
from jax import lax
from jax.experimental import pallas as pl
from jax.experimental.pallas import tpu as pltpu
from jax.sharding import Mesh
from jax.sharding import PartitionSpec as P

f32 = jnp.float32
bf16 = jnp.bfloat16

GROUP_DIM = 256
HEAD_DIM = 128
CHUNK = 256
RIM = 16
EPS = 1e-06
SP = ("sp_0", "sp_1")
FS_SP_TP = ("fs", "sp_0", "sp_1", "tp")
LONG, SHORT = 32, 32


def mm(a, b):
    return lax.dot_general(a, b, (((1,), (0,)), ((), ())), preferred_element_type=f32)


def mm_t(a, b):
    return lax.dot_general(a, b, (((1,), (1,)), ((), ())), preferred_element_type=f32)


def t_mm(a, b):
    return lax.dot_general(a, b, (((0,), (0,)), ((), ())), preferred_element_type=f32)


def call(body, outs, ins, scratch, limit_mib, flops, args, name):
    vm = pl.BlockSpec(memory_space=pltpu.VMEM)
    any_ = pl.BlockSpec(memory_space=pl.ANY)
    nbytes = sum(int(np.prod(a.shape)) * a.dtype.itemsize for a in args)
    return pl.pallas_call(
        body,
        out_shape=outs,
        in_specs=[any_ if kind == "a" else vm for kind in ins],
        out_specs=jax.tree.map(lambda _: vm, outs),
        scratch_shapes=scratch,
        compiler_params=pltpu.CompilerParams(vmem_limit_bytes=limit_mib << 20),
        cost_estimate=pl.CostEstimate(flops=int(flops), bytes_accessed=nbytes, transcendentals=0),
        name=name,
    )(*args)


def sds(shape, dtype):
    return jax.ShapeDtypeStruct(shape, dtype)


class Dims:
    def __init__(self, rows, width, heads, total_heads, seq):
        self.rows, self.width, self.heads = rows, width, heads
        self.chunks = rows // CHUNK
        self.block = 2 * rows
        base = [-(2.0**-5) * (seq / 16.0) ** (-2.0 * h / (total_heads - 1)) for h in range(total_heads)]
        self.logd = [float(np.float32(v)) for v in base]

    def log_decay(self, tp, h):
        return jnp.where(tp == 0, f32(self.logd[h]), f32(self.logd[h + self.heads]))


def decay(l, steps):
    return jnp.exp(jnp.full((1, HEAD_DIM), l * steps, f32))


def normalize(x_ref, gain_ref, out_ref):
    rows = x_ref.shape[0]
    step = 16

    @pl.loop(0, rows // step, unroll=4)
    def _(i):
        at = pl.ds(pl.multiple_of(i * step, step), step)
        x = x_ref[at, :].astype(f32)
        ms = jnp.mean(x * x, axis=-1, keepdims=True)
        out_ref[at, :] = (x * lax.rsqrt(ms + EPS) * gain_ref[...]).astype(bf16)


def angle_tables(a_cos, a_sin, b_cos, b_sin, cos_ref, sin_ref):
    c2, s2 = b_cos[...], b_sin[...]
    for a in range(a_cos.shape[0]):
        c1, s1 = a_cos[a : a + 1, :], a_sin[a : a + 1, :]
        at = slice(a * SHORT, (a + 1) * SHORT)
        cos_ref[at, :] = c1 * c2 - s1 * s2
        sin_ref[at, :] = s1 * c2 + c1 * s2


def row_scale(l):
    steps = lax.broadcasted_iota(jnp.int32, (CHUNK, HEAD_DIM), 0).astype(f32)
    return jnp.exp(l * steps)


def rotate_heads(d, xn_ref, w_ref, cos_ref, sin_ref, tp, sign, scale, out_ref):
    for pair in range(d.heads // 2):
        cols = slice(pair * 2 * HEAD_DIM, (pair + 1) * 2 * HEAD_DIM)
        acc = mm(xn_ref[...], w_ref[:, cols])
        for hh in range(2):
            h = 2 * pair + hh
            x = acc[:, hh * HEAD_DIM : (hh + 1) * HEAD_DIM].astype(bf16).astype(f32)
            y = x * cos_ref[...] + pltpu.roll(x, HEAD_DIM // 2, 1) * sin_ref[...]
            r = row_scale(sign * d.log_decay(tp, h)) * scale
            for c in range(d.chunks):
                at = slice(c * CHUNK, (c + 1) * CHUNK)
                out_ref[at, h * HEAD_DIM : (h + 1) * HEAD_DIM] = (y[at] * r).astype(bf16)


def centering():
    i = lax.broadcasted_iota(jnp.int32, (2 * HEAD_DIM, 2 * HEAD_DIM), 0)
    j = lax.broadcasted_iota(jnp.int32, (2 * HEAD_DIM, 2 * HEAD_DIM), 1)
    same = (i // HEAD_DIM) == (j // HEAD_DIM)
    mean = jnp.where(same, f32(1.0 / HEAD_DIM), f32(0.0))
    return i, j, mean


def centred_values(d, xn_ref, w_ref, out_ref):
    i, j, mean = centering()
    keep = (jnp.where(i == j, f32(1.0), f32(0.0)) - mean).astype(bf16)
    for pair in range(d.heads // 2):
        cols = slice(pair * 2 * HEAD_DIM, (pair + 1) * 2 * HEAD_DIM)
        v = mm(xn_ref[...], w_ref[:, cols]).astype(bf16)
        out_ref[:, cols] = mm(v, keep).astype(bf16)


def chunk_states(d, k_ref, v_ref, tp, u_ref):
    for h in range(d.heads):
        cols = slice(h * HEAD_DIM, (h + 1) * HEAD_DIM)
        last = decay(d.log_decay(tp, h), CHUNK - 1.0)
        for c in range(d.chunks):
            at = slice(c * CHUNK, (c + 1) * CHUNK)
            u_ref[c, h] = t_mm(k_ref[at, cols], v_ref[at, cols]) * last


def inside_chunks(d, q_ref, k_ref, v_ref, o_ref):
    i = lax.broadcasted_iota(jnp.int32, (CHUNK, CHUNK), 0)
    j = lax.broadcasted_iota(jnp.int32, (CHUNK, CHUNK), 1)
    causal = i >= j
    for c in range(d.chunks):
        at = slice(c * CHUNK, (c + 1) * CHUNK)
        for h in range(d.heads):
            cols = slice(h * HEAD_DIM, (h + 1) * HEAD_DIM)
            s = jnp.where(causal, mm_t(q_ref[at, cols], k_ref[at, cols]), 0.0).astype(bf16)
            o_ref[at, cols] = mm(s, v_ref[at, cols])


def load(src, dst, sem):
    copy = pltpu.make_async_copy(src, dst, sem)
    copy.start()
    return copy


def own_rows(
    d, x_hbm, gain, tc, ts, bc, bs, wk_hbm, wv_hbm, wq_hbm,
    xn, q_out, u_out, o_out, x, wk, wv, wq, k, v, ac, as_, cos, sin, sems,
):
    tp = lax.axis_index("tp")
    sp = lax.axis_index("sp_0") * 4 + lax.axis_index("sp_1")
    n = d.rows // LONG
    first = pl.multiple_of((sp * 2 + tp) * n, n)
    cx = load(x_hbm, x, sems.at[0])
    c1 = load(tc.at[pl.ds(first, n)], ac, sems.at[1])
    c2 = load(ts.at[pl.ds(first, n)], as_, sems.at[2])
    ck = load(wk_hbm, wk, sems.at[3])
    cv = load(wv_hbm, wv, sems.at[4])
    cq = load(wq_hbm, wq, sems.at[5])
    c1.wait()
    c2.wait()
    angle_tables(ac, as_, bc, bs, cos, sin)
    cx.wait()
    normalize(x, gain, xn)
    ck.wait()
    rotate_heads(d, xn, wk, cos, sin, tp, -1.0, HEAD_DIM**-0.5, k)
    cv.wait()
    centred_values(d, xn, wv, v)
    chunk_states(d, k, v, tp, u_out)
    cq.wait()
    rotate_heads(d, xn, wq, cos, sin, tp, 1.0, 1.0, q_out)
    inside_chunks(d, q_out, k, v, o_out)


def partner_keys(
    d, x_hbm, gain, tc, ts, bc, bs, wk_hbm, wv_hbm, u_own,
    xn, k_out, v_out, u_out, s_out, cos, sin, x, wk, wv, ac, as_, sems,
):
    tp = lax.axis_index("tp")
    sp = lax.axis_index("sp_0") * 4 + lax.axis_index("sp_1")
    n = d.rows // LONG
    first = pl.multiple_of((sp * 2 + 1 - tp) * n, n)
    cx = load(x_hbm, x, sems.at[0])
    c1 = load(tc.at[pl.ds(first, n)], ac, sems.at[1])
    c2 = load(ts.at[pl.ds(first, n)], as_, sems.at[2])
    ck = load(wk_hbm, wk, sems.at[3])
    cv = load(wv_hbm, wv, sems.at[4])
    c1.wait()
    c2.wait()
    angle_tables(ac, as_, bc, bs, cos, sin)
    cx.wait()
    normalize(x, gain, xn)
    ck.wait()
    rotate_heads(d, xn, wk, cos, sin, tp, -1.0, HEAD_DIM**-0.5, k_out)
    cv.wait()
    centred_values(d, xn, wv, v_out)
    chunk_states(d, k_out, v_out, tp, u_out)
    last = 2 * d.chunks - 1
    for h in range(d.heads):
        l = d.log_decay(tp, h)
        total = jnp.zeros((HEAD_DIM, HEAD_DIM), f32)
        for c in range(d.chunks):
            own = (last - c - tp * d.chunks).astype(f32) * CHUNK
            other = (last - c - (1 - tp) * d.chunks).astype(f32) * CHUNK
            total += decay(l, own) * u_own[c, h] + decay(l, other) * u_out[c, h]
        s_out[h * HEAD_DIM : (h + 1) * HEAD_DIM, :] = total.astype(bf16)


def partner_queries(
    d, xn_own, xn_par, k, v, cos, sin, wp_hbm, wq_hbm,
    pool_out, tail_out, q_out, o_out, wp, wq, sems,
):
    tp = lax.axis_index("tp")
    cp = load(wp_hbm, wp, sems.at[0])
    cq = load(wq_hbm, wq, sems.at[1])
    own = pl.multiple_of(tp * d.rows, d.rows)
    other = pl.multiple_of((1 - tp) * d.rows, d.rows)
    cp.wait()
    for at, xn in ((own, xn_own), (other, xn_par)):
        for t in range(d.width // 256):
            cols = slice(t * 256, (t + 1) * 256)
            pool_out[pl.ds(at, d.rows), cols] = mm(xn[...], wp[:, cols]).astype(bf16)
    tail_out[...] = pool_out[d.block - RIM :, :]
    cq.wait()
    rotate_heads(d, xn_par, wq, cos, sin, tp, 1.0, 1.0, q_out)
    inside_chunks(d, q_out, k, v, o_out)


def row_states(d, own, r1, r2, r3, total_out, prefix_out):
    tp = lax.axis_index("tp")
    y = lax.axis_index("sp_1")
    for h in range(d.heads):
        at = slice(h * HEAD_DIM, (h + 1) * HEAD_DIM)
        l = d.log_decay(tp, h)
        total = decay(l, (3 - y).astype(f32) * d.block) * own[at, :].astype(f32)
        prefix = jnp.zeros((HEAD_DIM, HEAD_DIM), f32)
        for k, r in ((1, r1), (2, r2), (3, r3)):
            part = r[at, :].astype(f32)
            behind = lax.rem(y - k + 4, 4)
            total += decay(l, (3 - behind).astype(f32) * d.block) * part
            prefix += jnp.where(y >= k, decay(l, (k - 1.0) * d.block), 0.0) * part
        total_out[at, :] = total.astype(bf16)
        prefix_out[at, :] = prefix


def gates_and_pools(
    d, xn_own, xn_par, pool_in, rim, mix, bias, gain, ret_gain, wg_hbm,
    g_own, g_par, p_own, p_par, wg, ext, po, sems,
):
    tp = lax.axis_index("tp")
    sp = lax.axis_index("sp_0") * 4 + lax.axis_index("sp_1")
    cg = load(wg_hbm, wg, sems.at[0])
    own = pl.multiple_of(tp * d.rows, d.rows)
    other = pl.multiple_of((1 - tp) * d.rows, d.rows)
    ext[0:RIM, :] = rim[...]
    ext[RIM:, :] = pool_in[...]
    i = lax.broadcasted_iota(jnp.int32, (CHUNK, CHUNK + RIM), 0) + RIM
    j = lax.broadcasted_iota(jnp.int32, (CHUNK, CHUNK + RIM), 1)
    groups = d.width // GROUP_DIM
    for g in range(groups):
        window = jnp.where(tp == 0, 2 ** (g + 1), 2 ** (g + 1 + groups))
        band = jnp.where((i >= j) & (i - j < window), f32(1.0), f32(0.0)).astype(bf16)
        cols = slice(g * GROUP_DIM, (g + 1) * GROUP_DIM)
        for c in range(2 * d.chunks):
            rows = slice(c * CHUNK, (c + 1) * CHUNK)
            t = lax.broadcasted_iota(jnp.int32, (CHUNK, 1), 0) + (sp * d.block + c * CHUNK + 1)
            count = jnp.minimum(t, window).astype(f32)
            sums = mm(band, ext[c * CHUNK : c * CHUNK + CHUNK + RIM, cols])
            diff = sums * (1.0 / count) - pool_in[rows, cols].astype(f32)
            mixed = mm(diff.astype(bf16), mix[g]) + bias[g : g + 1, :]
            po[rows, cols] = (mixed * gain[:, cols]).astype(bf16)
    p_own[...] = po[pl.ds(own, d.rows), :]
    p_par[...] = po[pl.ds(other, d.rows), :]
    cg.wait()
    for xn, out in ((xn_own, g_own), (xn_par, g_par)):
        for t in range(d.width // 256):
            cols = slice(t * 256, (t + 1) * 256)
            gate = mm(xn[...], wg[:, cols]).astype(bf16).astype(f32)
            out[:, cols] = (gate * jax.nn.sigmoid(gate) * ret_gain[:, cols]).astype(bf16)


def retention_rows(d, half, tp, q, o, gate, prefix, z1, z2, z3, u_own, u_par, out, s_ref):
    z = lax.axis_index("sp_0")
    y = lax.axis_index("sp_1")
    rowlen = 4.0 * d.block
    s_ref[...] = jnp.zeros_like(s_ref)
    for h in range(d.heads):
        at = slice(h * HEAD_DIM, (h + 1) * HEAD_DIM)
        l = d.log_decay(tp, h)
        rows_before = jnp.zeros((HEAD_DIM, HEAD_DIM), f32)
        for k, r in ((1, z1), (2, z2), (3, z3)):
            rows_before += jnp.where(z >= k, decay(l, (k - 1.0) * rowlen), 0.0) * r[at, :].astype(f32)
        incoming = prefix[at, :] + decay(l, y.astype(f32) * d.block) * rows_before
        sub = slice((h % 2) * HEAD_DIM, (h % 2 + 1) * HEAD_DIM)
        one = decay(l, 1.0)
        step = decay(l, float(CHUNK))
        after = incoming
        for c in range(d.chunks):
            u_first = jnp.where(tp == 0, u_own[c, h], u_par[c, h])
            after = step * after + u_first
        state = jnp.where(half == 0, incoming, after)
        for c in range(d.chunks):
            s_ref[c, h // 2, sub, sub] = (one * state).astype(bf16)
            if c + 1 < d.chunks:
                u_here = jnp.where(half == tp, u_own[c, h], u_par[c, h])
                state = step * state + u_here
    _, _, mean = centering()
    mean = mean.astype(bf16)
    for c in range(d.chunks):
        at = slice(c * CHUNK, (c + 1) * CHUNK)
        for pair in range(d.heads // 2):
            cols = slice(pair * 2 * HEAD_DIM, (pair + 1) * 2 * HEAD_DIM)
            raw = o[at, cols] + mm(q[at, cols], s_ref[c, pair])
            var = mm((raw * raw).astype(bf16), mean)
            ret = gate[at, cols].astype(f32) * (raw * lax.rsqrt(var + EPS))
            out[at, cols] = ret.astype(bf16)


def partner_retention(d, q, o, gate, prefix, z1, z2, z3, u_own, u_par, out, s_ref):
    tp = lax.axis_index("tp")
    retention_rows(d, 1 - tp, tp, q, o, gate, prefix, z1, z2, z3, u_own, u_par, out, s_ref)


def pool_outputs(d, p_own, p_recv, w_own_hbm, w_par_hbm, acc, w_own, w_par, sems):
    co = load(w_own_hbm, w_own, sems.at[0])
    cp = load(w_par_hbm, w_par, sems.at[1])
    co.wait()
    cp.wait()
    for t in range(acc.shape[1] // 256):
        cols = slice(t * 256, (t + 1) * 256)
        acc[:, cols] = mm(p_own[...], w_own[:, cols]) + mm(p_recv[...], w_par[:, cols])


def own_retention(
    d, q, o, gate, prefix, z1, z2, z3, u_own, u_par, acc_in, w_hbm, acc, s_ref, ret, w, sems
):
    tp = lax.axis_index("tp")
    cw = load(w_hbm, w, sems.at[0])
    retention_rows(d, tp, tp, q, o, gate, prefix, z1, z2, z3, u_own, u_par, ret, s_ref)
    cw.wait()
    for t in range(acc.shape[1] // 256):
        cols = slice(t * 256, (t + 1) * 256)
        acc[:, cols] = acc_in[:, cols] + mm(ret[...], w[:, cols])


def last_share(d, acc_in, ret, w_hbm, out, w, sems):
    cw = load(w_hbm, w, sems.at[0])
    cw.wait()
    for t in range(out.shape[1] // 256):
        cols = slice(t * 256, (t + 1) * 256)
        out[:, cols] = (acc_in[:, cols] + mm(ret[...], w[:, cols])).astype(bf16)


def swap(x):
    return lax.ppermute(x, "tp", [(0, 1), (1, 0)])


def per_device(
    seq, tokens, norm_gain, w_pool, w_query, w_key, w_value, w_gate, pool_mix, pool_bias,
    pool_gain, ret_gain, w_out_pool, w_out_ret,
):
    rows, model = tokens.shape
    width = w_query.shape[1]
    heads = width // HEAD_DIM
    d = Dims(rows, width, heads, heads * 2, seq)
    n = rows // LONG
    dma = pltpu.SemaphoreType.DMA
    vmem = pltpu.VMEM
    gain = norm_gain[None, :]

    half = HEAD_DIM // 2
    freq = 10000.0 ** (-np.arange(half, dtype=np.float64) / half)
    freq = np.concatenate([freq, freq])
    sign = np.concatenate([-np.ones(half), np.ones(half)])
    a = np.arange(seq // LONG)[:, None] * float(LONG) * freq
    b = np.arange(SHORT)[:, None] * freq
    tc, ts = np.cos(a).astype(np.float32), (np.sin(a) * sign).astype(np.float32)
    bc, bs = np.cos(b).astype(np.float32), (np.sin(b) * sign).astype(np.float32)

    proj = 2.0 * rows * model * width
    other_tokens = swap(tokens)
    u_shape = sds((d.chunks, heads, HEAD_DIM, HEAD_DIM), f32)
    act = sds((rows, width), bf16)
    xn_own, q_own, u_own, o_own = call(
        functools.partial(own_rows, d),
        [sds((rows, model), bf16), act, u_shape, sds((rows, width), f32)],
        "avaavvaaa",
        [
            vmem((rows, model), bf16), vmem((model, width), bf16), vmem((model, width), bf16),
            vmem((model, width), bf16), vmem((rows, width), bf16), vmem((rows, width), bf16),
            vmem((n, HEAD_DIM), f32), vmem((n, HEAD_DIM), f32), vmem((rows, HEAD_DIM), f32),
            vmem((rows, HEAD_DIM), f32), dma((6,)),
        ],
        28, 3.6 * proj, (tokens, gain, tc, ts, bc, bs, w_key, w_value, w_query), "own_rows",
    )
    other_pool_w = swap(w_out_pool)
    other_ret_w = swap(w_out_ret)
    xn_par, k_par, v_par, u_par, state, cos, sin = call(
        functools.partial(partner_keys, d),
        [
            sds((rows, model), bf16), act, act, u_shape, sds((width, HEAD_DIM), bf16),
            sds((rows, HEAD_DIM), f32), sds((rows, HEAD_DIM), f32),
        ],
        "avaavvaav",
        [
            vmem((rows, model), bf16), vmem((model, width), bf16), vmem((model, width), bf16),
            vmem((n, HEAD_DIM), f32), vmem((n, HEAD_DIM), f32), dma((5,)),
        ],
        24, 2.4 * proj, (other_tokens, gain, tc, ts, bc, bs, w_key, w_value, u_own), "partner_keys",
    )
    ys = [lax.ppermute(state, "sp_1", [(i, (i + k) % 4) for i in range(4)]) for k in (1, 2, 3)]
    pool_in, tail, q_par, o_par = call(
        functools.partial(partner_queries, d),
        [sds((d.block, width), bf16), sds((RIM, width), bf16), act, sds((rows, width), f32)],
        "vvvvvvaa",
        [vmem((model, width), bf16), vmem((model, width), bf16), dma((2,))],
        24, 3.4 * proj, (xn_own, xn_par, k_par, v_par, cos, sin, w_pool, w_query), "partner_queries",
    )
    rim = lax.ppermute(tail, SP, [(i, i + 1) for i in range(seq // d.block - 1)])
    total, prefix = call(
        functools.partial(row_states, d),
        [sds((width, HEAD_DIM), bf16), sds((width, HEAD_DIM), f32)],
        "vvvv", [], 4, 0.1 * proj, (state, *ys), "row_states",
    )
    zs = [lax.ppermute(total, "sp_0", [(i, i + k) for i in range(4 - k)]) for k in (1, 2, 3)]
    g_own, g_par, p_own, p_par = call(
        functools.partial(gates_and_pools, d),
        [act, act, act, act],
        "vvvvvvvva",
        [
            vmem((model, width), bf16), vmem((d.block + RIM, width), bf16),
            vmem((d.block, width), bf16), dma((1,)),
        ],
        24, 2.8 * proj,
        (xn_own, xn_par, pool_in, rim, pool_mix, pool_bias, pool_gain[None], ret_gain[None], w_gate),
        "gates_and_pools",
    )
    p_recv = swap(p_par)
    acc = call(
        functools.partial(pool_outputs, d),
        sds((rows, model), f32), "vvaa",
        [vmem((width, model), bf16), vmem((width, model), bf16), dma((2,))],
        16, 2.0 * proj, (p_own, p_recv, w_out_pool, other_pool_w), "pool_outputs",
    )
    s_scratch = vmem((d.chunks, heads // 2, 2 * HEAD_DIM, 2 * HEAD_DIM), bf16)
    ret_par = call(
        functools.partial(partner_retention, d),
        act, "vvvvvvvvv", [s_scratch], 12, 0.5 * proj,
        (q_par, o_par, g_par, prefix, *zs, u_own, u_par), "partner_retention",
    )
    ret_recv = swap(ret_par)
    acc = call(
        functools.partial(own_retention, d),
        sds((rows, model), f32), "vvvvvvvvvva",
        [s_scratch, vmem((rows, width), bf16), vmem((width, model), bf16), dma((1,))],
        20, 1.5 * proj,
        (q_own, o_own, g_own, prefix, *zs, u_own, u_par, acc, w_out_ret), "own_retention",
    )
    return call(
        functools.partial(last_share, d),
        sds((rows, model), bf16), "vva",
        [vmem((width, model), bf16), dma((1,))],
        16, 1.0 * proj, (acc, ret_recv, other_ret_w), "last_share",
    )


def solution(mesh):
    finer = Mesh(
        mesh.devices.reshape(4, 4, mesh.shape["fs"], mesh.shape["tp"]), ("sp_0", "sp_1", "fs", "tp")
    )
    placed = (
        P(FS_SP_TP, None), P(), P(None, "tp"), P(None, "tp"), P(None, "tp"), P(None, "tp"),
        P(None, "tp"), P("tp", None, None), P("tp", None), P("tp"), P("tp"), P("tp", None),
        P("tp", None),
    )

    def whole(tokens, *rest):
        seq = tokens.shape[0] // mesh.shape["fs"]
        return jax.shard_map(
            functools.partial(per_device, seq), mesh=finer, in_specs=placed,
            out_specs=P(FS_SP_TP, None), check_vma=False,
        )(tokens, *rest)

    return whole
```

```python
import functools

import jax
import jax.numpy as jnp
import numpy as np
from jax import lax
from jax.experimental import pallas as pl
from jax.experimental.pallas import tpu as pltpu
from jax.sharding import Mesh
from jax.sharding import PartitionSpec as P


f32 = jnp.float32
bf16 = jnp.bfloat16

GROUP_DIM = 256
HEAD_DIM = 128
CHUNK = 256
RIM = 16
EPS = 1e-06
SP = ("sp_0", "sp_1")
FS_SP_TP = ("fs", "sp_0", "sp_1", "tp")
LONG, SHORT = 32, 32


def mm(a, b):
    return lax.dot_general(a, b, (((1,), (0,)), ((), ())), preferred_element_type=f32)


def mm_t(a, b):
    return lax.dot_general(a, b, (((1,), (1,)), ((), ())), preferred_element_type=f32)


def t_mm(a, b):
    return lax.dot_general(a, b, (((0,), (0,)), ((), ())), preferred_element_type=f32)


def with_loads(body, ins, outs, loads):
    def wrapped(*refs):
        first, rest = refs[:ins], refs[ins:]
        sources, rest = rest[:loads], rest[loads:]
        results, rest = rest[:outs], rest[outs:]
        targets, rest = rest[:loads], rest[loads:]
        copies = [
            pltpu.make_async_copy(source, target, rest[-1].at[i])
            for i, (source, target) in enumerate(zip(sources, targets))
        ]
        for copy in copies:
            copy.start()
        body(*first, *results, *rest[:-1])
        for copy in copies:
            copy.wait()

    return wrapped


def call(body, outs, ins, scratch, limit_mib, flops, args, outs_hbm=False, loads=()):
    vm = pl.BlockSpec(memory_space=pltpu.VMEM)
    hbm = pl.BlockSpec(memory_space=pltpu.HBM)
    if loads:
        outs = list(outs) if isinstance(outs, (list, tuple)) else [outs]
        body = with_loads(body, len(ins), len(outs), len(loads))
        ins += "h" * len(loads)
        args = (*args, *loads)
        outs = outs + [sds(a.shape, a.dtype) for a in loads]
        scratch = [*scratch, pltpu.SemaphoreType.DMA((len(loads),))]
    args = [
        pltpu.with_memory_space_constraint(a, pltpu.HBM) if kind == "h" else a
        for a, kind in zip(args, ins)
    ]
    nbytes = sum(int(np.prod(a.shape)) * a.dtype.itemsize for a in args)
    return pl.pallas_call(
        body,
        out_shape=outs,
        in_specs=[hbm if kind == "h" else vm for kind in ins],
        out_specs=jax.tree.map(lambda _: hbm if outs_hbm else vm, outs),
        scratch_shapes=scratch,
        compiler_params=pltpu.CompilerParams(vmem_limit_bytes=limit_mib << 20),
        cost_estimate=pl.CostEstimate(flops=int(flops), bytes_accessed=nbytes, transcendentals=0),
    )(*args)


def sds(shape, dtype):
    return jax.ShapeDtypeStruct(shape, dtype)


def normed_f32(rows, model):
    return sds((rows, model), f32)


class Dims:
    def __init__(self, rows, width, heads, total_heads, seq):
        self.rows, self.width, self.heads = rows, width, heads
        self.chunks = rows // CHUNK
        self.block = 2 * rows
        base = [-(2.0**-5) * (seq / 16.0) ** (-2.0 * h / (total_heads - 1)) for h in range(total_heads)]
        self.logd = [float(np.float32(v)) for v in base]

    def log_decay(self, tp, h):
        return jnp.where(tp == 0, f32(self.logd[h]), f32(self.logd[h + self.heads]))


def decay(l, steps):
    return jnp.exp(jnp.full((1, HEAD_DIM), l * steps, f32))


def normalize(x_ref, gain_ref, out_ref, lo, hi):
    for at in range(lo, hi, RIM):
        x = x_ref[at : at + RIM, :].astype(f32)
        ms = jnp.mean(x * x, axis=-1, keepdims=True)
        out_ref[at : at + RIM, :] = (x * lax.rsqrt(ms + EPS) * gain_ref[...]).astype(bf16)


def angle_tables(a_cos, a_sin, b_cos, b_sin, cos_ref, sin_ref):
    c2, s2 = b_cos[...], b_sin[...]
    for a in range(a_cos.shape[0]):
        c1, s1 = a_cos[a : a + 1, :], a_sin[a : a + 1, :]
        at = slice(a * SHORT, (a + 1) * SHORT)
        cos_ref[at, :] = c1 * c2 - s1 * s2
        sin_ref[at, :] = s1 * c2 + c1 * s2


def row_scales(d, tp, pos, neg):
    steps = lax.broadcasted_iota(jnp.int32, (8, HEAD_DIM), 0).astype(f32)
    for h in range(d.heads):
        l = d.log_decay(tp, h)
        for sign, scale, out in ((1.0, 1.0, pos), (-1.0, HEAD_DIM**-0.5, neg)):
            now = jnp.exp(sign * l * steps) * scale
            step = decay(sign * l, 8.0)
            for i in range(CHUNK // 8):
                out[h, i * 8 : i * 8 + 8, :] = now
                now = now * step


def rotate_heads(d, acc, cos_ref, sin_ref, scales, out_ref):
    for c in range(d.chunks):
        at = slice(c * CHUNK, (c + 1) * CHUNK)
        for h in range(d.heads):
            cols = slice(h * HEAD_DIM, (h + 1) * HEAD_DIM)
            x = acc[at, cols]
            y = x * cos_ref[at, :] + pltpu.roll(x, HEAD_DIM // 2, 1) * sin_ref[at, :]
            out_ref[at, cols] = (y * scales[h]).astype(bf16)


def centering():
    i = lax.broadcasted_iota(jnp.int32, (2 * HEAD_DIM, 2 * HEAD_DIM), 0)
    j = lax.broadcasted_iota(jnp.int32, (2 * HEAD_DIM, 2 * HEAD_DIM), 1)
    same = (i // HEAD_DIM) == (j // HEAD_DIM)
    mean = jnp.where(same, f32(1.0 / HEAD_DIM), f32(0.0))
    return i, j, mean


def centred_values(d, v_raw, out_ref):
    i, j, mean = centering()
    keep = (jnp.where(i == j, f32(1.0), f32(0.0)) - mean).astype(bf16)
    for pair in range(d.heads // 2):
        cols = slice(pair * 2 * HEAD_DIM, (pair + 1) * 2 * HEAD_DIM)
        out_ref[:, cols] = mm(v_raw[:, cols], keep).astype(bf16)


def chunk_states(d, k_ref, v_ref, tp, u_ref):
    for h in range(d.heads):
        cols = slice(h * HEAD_DIM, (h + 1) * HEAD_DIM)
        last = decay(d.log_decay(tp, h), CHUNK - 1.0)
        for c in range(d.chunks):
            at = slice(c * CHUNK, (c + 1) * CHUNK)
            u_ref[c, h] = t_mm(k_ref[at, cols], v_ref[at, cols]) * last


def inside_chunks(d, q_ref, k_ref, v_ref, o_ref):
    i = lax.broadcasted_iota(jnp.int32, (CHUNK, CHUNK), 0)
    j = lax.broadcasted_iota(jnp.int32, (CHUNK, CHUNK), 1)
    causal = i >= j
    for c in range(d.chunks):
        at = slice(c * CHUNK, (c + 1) * CHUNK)
        for h in range(d.heads):
            cols = slice(h * HEAD_DIM, (h + 1) * HEAD_DIM)
            s = jnp.where(causal, mm_t(q_ref[at, cols], k_ref[at, cols]), 0.0).astype(bf16)
            o_ref[at, cols] = mm(s, v_ref[at, cols])


def load(src, dst, sem):
    copy = pltpu.make_async_copy(src, dst, sem)
    copy.start()
    return copy


def place(d, half):
    sp = lax.axis_index("sp_0") * 4 + lax.axis_index("sp_1")
    n = d.rows // LONG
    return pl.ds(pl.multiple_of((sp * 2 + half) * n, n), n)


def own_keys(
    d, x_hbm, gain_hbm, tc, ts, bc_hbm, bs_hbm, wk_hbm, wv_hbm,
    xn, k, v, u_out, cos, sin, cos_par, sin_par, wk, wv, gain, pos, neg,
    x, ac, as_, bc, bs, acc, v_raw, sems,
):
    tp = lax.axis_index("tp")
    mid = d.rows // 2
    halves = (slice(0, mid), slice(mid, d.rows))
    small = [load(gain_hbm, gain, sems.at[0])]
    cx0 = load(x_hbm.at[halves[0]], x.at[halves[0]], sems.at[1])
    cx1 = load(x_hbm.at[halves[1]], x.at[halves[1]], sems.at[2])
    ck = load(wk_hbm, wk, sems.at[3])
    small += [
        load(bc_hbm, bc, sems.at[4]),
        load(bs_hbm, bs, sems.at[5]),
        load(tc.at[place(d, tp)], ac.at[0], sems.at[6]),
        load(ts.at[place(d, tp)], as_.at[0], sems.at[7]),
        load(tc.at[place(d, 1 - tp)], ac.at[1], sems.at[8]),
        load(ts.at[place(d, 1 - tp)], as_.at[1], sems.at[9]),
    ]
    cv = load(wv_hbm, wv, sems.at[10])
    row_scales(d, tp, pos, neg)
    small[0].wait()
    cx0.wait()
    normalize(x, gain, xn, 0, mid)
    cx1.wait()
    normalize(x, gain, xn, mid, d.rows)
    ck.wait()
    acc[...] = mm(xn[...], wk[...])
    for copy in small[1:]:
        copy.wait()
    cv.wait()
    angle_tables(ac.at[0], as_.at[0], bc, bs, cos, sin)
    angle_tables(ac.at[1], as_.at[1], bc, bs, cos_par, sin_par)
    v_raw[...] = mm(xn[...], wv[...]).astype(bf16)
    rotate_heads(d, acc, cos, sin, neg, k)
    centred_values(d, v_raw, v)
    chunk_states(d, k, v, tp, u_out)


def partner_keys(
    d, x, gain, cos, sin, wk, wv, neg, u_own, xn, k, v, u_out, s_out, acc, v_raw
):
    tp = lax.axis_index("tp")
    mid = d.rows // 2
    normalize(x, gain, xn, 0, mid)
    acc[0:mid, :] = mm(xn[0:mid, :], wk[...])
    normalize(x, gain, xn, mid, d.rows)
    acc[mid:, :] = mm(xn[mid:, :], wk[...])
    v_raw[...] = mm(xn[...], wv[...]).astype(bf16)
    rotate_heads(d, acc, cos, sin, neg, k)
    centred_values(d, v_raw, v)
    chunk_states(d, k, v, tp, u_out)
    last = 2 * d.chunks - 1
    for h in range(d.heads):
        l = d.log_decay(tp, h)
        total = jnp.zeros((HEAD_DIM, HEAD_DIM), f32)
        for c in range(d.chunks):
            own = (last - c - tp * d.chunks).astype(f32) * CHUNK
            other = (last - c - (1 - tp) * d.chunks).astype(f32) * CHUNK
            total += decay(l, own) * u_own[c, h] + decay(l, other) * u_out[c, h]
        s_out[h * HEAD_DIM : (h + 1) * HEAD_DIM, :] = total.astype(bf16)


def pool_inputs(d, xn_own, xn_par, wp, pool_out, tail_out):
    tp = lax.axis_index("tp")
    own = pl.multiple_of(tp * d.rows, d.rows)
    other = pl.multiple_of((1 - tp) * d.rows, d.rows)
    for at, xn in ((own, xn_own), (other, xn_par)):
        for t in range(d.width // 256):
            cols = slice(t * 256, (t + 1) * 256)
            pool_out[pl.ds(at, d.rows), cols] = mm(xn[...], wp[:, cols]).astype(bf16)
    tail_out[...] = pool_out[d.block - RIM :, :]


def queries(d, xn, k, v, cos, sin, pos, wq, q, o, acc):
    acc[...] = mm(xn[...], wq[...])
    rotate_heads(d, acc, cos, sin, pos, q)
    inside_chunks(d, q, k, v, o)


def heads_of(d):
    for h in range(d.heads):
        yield h, slice(h * HEAD_DIM, (h + 1) * HEAD_DIM)


def pair_states(d, own, got, out):
    tp = lax.axis_index("tp")
    odd = lax.rem(lax.axis_index("sp_1"), 2) == 1
    for h, at in heads_of(d):
        step = decay(d.log_decay(tp, h), 1.0 * d.block)
        a, b = own[at, :].astype(f32), got[at, :].astype(f32)
        out[at, :] = (jnp.where(odd, step * b + a, step * a + b)).astype(bf16)


def row_states(d, got1, pair, got2, out, prefix_out):
    tp = lax.axis_index("tp")
    y = lax.axis_index("sp_1")
    for h, at in heads_of(d):
        l = d.log_decay(tp, h)
        a, b = pair[at, :].astype(f32), got2[at, :].astype(f32)
        two = decay(l, 2.0 * d.block)
        out[at, :] = jnp.where(y >= 2, two * b + a, two * a + b).astype(bf16)
        one = jnp.where(lax.rem(y, 2) == 1, got1[at, :].astype(f32), 0.0)
        far = jnp.where(y >= 2, decay(l, (y - 2).astype(f32) * d.block), 0.0)
        prefix_out[at, :] = one + far * b


def column_states(d, own, got, out):
    tp = lax.axis_index("tp")
    odd = lax.rem(lax.axis_index("sp_0"), 2) == 1
    for h, at in heads_of(d):
        step = decay(d.log_decay(tp, h), 4.0 * d.block)
        a, b = own[at, :].astype(f32), got[at, :].astype(f32)
        out[at, :] = (jnp.where(odd, step * b + a, step * a + b)).astype(bf16)


def pools(d, pool_in, rim, mix, bias, gain, p_own, p_par, ext, diff, po):
    tp = lax.axis_index("tp")
    sp = lax.axis_index("sp_0") * 4 + lax.axis_index("sp_1")
    own = pl.multiple_of(tp * d.rows, d.rows)
    other = pl.multiple_of((1 - tp) * d.rows, d.rows)
    ext[0:RIM, :] = jnp.where(sp > 0, rim[...].astype(f32), 0.0).astype(bf16)
    ext[RIM:, :] = pool_in[...]
    i = lax.broadcasted_iota(jnp.int32, (CHUNK, CHUNK + RIM), 0) + RIM
    j = lax.broadcasted_iota(jnp.int32, (CHUNK, CHUNK + RIM), 1)
    groups = d.width // GROUP_DIM
    chunks = 2 * d.chunks
    for g in range(groups):
        window = jnp.where(tp == 0, 2 ** (g + 1), 2 ** (g + 1 + groups))
        band = jnp.where((i >= j) & (i - j < window), f32(1.0), f32(0.0)).astype(bf16)
        cols = slice(g * GROUP_DIM, (g + 1) * GROUP_DIM)
        blocks = [ext[c * CHUNK : c * CHUNK + CHUNK + RIM, cols] for c in range(chunks)]
        sums = mm(band, jnp.concatenate(blocks, axis=1))
        for c in range(chunks):
            rows = slice(c * CHUNK, (c + 1) * CHUNK)
            t = lax.broadcasted_iota(jnp.int32, (CHUNK, GROUP_DIM), 0) + (sp * d.block + c * CHUNK + 1)
            part = sums[:, c * GROUP_DIM : (c + 1) * GROUP_DIM]
            if c == 0:
                share = 1.0 / jnp.minimum(t, window).astype(f32)
            else:
                share = 1.0 / window.astype(f32)
            diff[rows, cols] = (part * share - pool_in[rows, cols].astype(f32)).astype(bf16)
    for g in range(groups):
        cols = slice(g * GROUP_DIM, (g + 1) * GROUP_DIM)
        mixed = mm(diff[:, cols], mix[g]) + bias[g : g + 1, :]
        po[:, cols] = (mixed * gain[:, cols]).astype(bf16)
    p_own[...] = po[pl.ds(own, d.rows), :]
    p_par[...] = po[pl.ds(other, d.rows), :]


def gates(xn, ret_gain, wg, out):
    gate = mm(xn[...], wg[...])
    out[...] = (gate * jax.nn.sigmoid(gate) * ret_gain[...]).astype(bf16)


def chunk_bases(d, prefix, got3, u_own, u_par, own_out, par_out):
    tp, z, y = lax.axis_index("tp"), lax.axis_index("sp_0"), lax.axis_index("sp_1")
    for h, at in heads_of(d):
        l = d.log_decay(tp, h)
        row_before = jnp.where(lax.rem(z, 2) == 1, got3[at, :].astype(f32), 0.0)
        state = prefix[at, :] + decay(l, y.astype(f32) * d.block) * row_before
        one, step = decay(l, 1.0), decay(l, float(CHUNK))
        states = []
        for g in range(2 * d.chunks):
            states.append(state)
            own, par = u_own[g % d.chunks, h], u_par[g % d.chunks, h]
            state = step * state + jnp.where(tp == g // d.chunks, own, par)
        for c in range(d.chunks):
            first, second = one * states[c], one * states[c + d.chunks]
            own_out[c, h] = jnp.where(tp == 0, first, second)
            par_out[c, h] = jnp.where(tp == 0, second, first)


def retention_rows(d, half, tp, q, o, gate, base, got4, out, s_ref):
    z, y = lax.axis_index("sp_0"), lax.axis_index("sp_1")
    before = (z - 2) * (4 * d.block) + y * d.block + half * d.rows + 1
    none = jnp.zeros((HEAD_DIM, HEAD_DIM), bf16)
    for h, at in heads_of(d):
        l = d.log_decay(tp, h)
        sub = slice((h % 2) * HEAD_DIM, (h % 2 + 1) * HEAD_DIM)
        rest = slice((1 - h % 2) * HEAD_DIM, (2 - h % 2) * HEAD_DIM)
        far = got4[at, :].astype(f32)
        for c in range(d.chunks):
            steps = jnp.maximum(before + c * CHUNK, 0).astype(f32)
            share = jnp.where(z >= 2, decay(l, steps), 0.0)
            s_ref[c, h // 2, sub, sub] = (base[c, h] + share * far).astype(bf16)
            s_ref[c, h // 2, sub, rest] = none
    _, _, mean = centering()
    mean = mean.astype(bf16)
    for c in range(d.chunks):
        at = slice(c * CHUNK, (c + 1) * CHUNK)
        for pair in range(d.heads // 2):
            cols = slice(pair * 2 * HEAD_DIM, (pair + 1) * 2 * HEAD_DIM)
            raw = o[at, cols] + mm(q[at, cols], s_ref[c, pair])
            var = mm((raw * raw).astype(bf16), mean)
            ret = gate[at, cols].astype(f32) * (raw * lax.rsqrt(var + EPS))
            out[at, cols] = ret.astype(bf16)


def partner_retention(d, q, o, gate, base, got4, out, s_ref):
    tp = lax.axis_index("tp")
    retention_rows(d, 1 - tp, tp, q, o, gate, base, got4, out, s_ref)


def pool_outputs(p_own, p_recv, w_own, w_par, acc):
    for t in range(acc.shape[1] // 512):
        cols = slice(t * 512, (t + 1) * 512)
        acc[:, cols] = mm(p_own[...], w_own[:, cols]) + mm(p_recv[...], w_par[:, cols])


def own_retention(d, q, o, gate, base, got4, acc_in, w, acc, s_ref, ret):
    tp = lax.axis_index("tp")
    retention_rows(d, tp, tp, q, o, gate, base, got4, ret, s_ref)
    for t in range(acc.shape[1] // 256):
        cols = slice(t * 256, (t + 1) * 256)
        acc[:, cols] = acc_in[:, cols] + mm(ret[...], w[:, cols])


def last_share(acc_in, ret, w, out_hbm, out, sems):
    copies = []
    step = 512
    for t in range(out.shape[1] // step):
        cols = slice(t * step, (t + 1) * step)
        out[:, cols] = (acc_in[:, cols] + mm(ret[...], w[:, cols])).astype(bf16)
        copies.append(pltpu.make_async_copy(out.at[:, cols], out_hbm.at[:, cols], sems.at[t]))
        copies[-1].start()
    for copy in copies:
        copy.wait()


def swap(x):
    return lax.ppermute(x, "tp", [(0, 1), (1, 0)])


def per_device(
    seq, tokens, norm_gain, w_pool, w_query, w_key, w_value, w_gate, pool_mix, pool_bias,
    pool_gain, ret_gain, w_out_pool, w_out_ret,
):
    rows, model = tokens.shape
    width = w_query.shape[1]
    heads = width // HEAD_DIM
    d = Dims(rows, width, heads, heads * 2, seq)
    n = rows // LONG
    dma = pltpu.SemaphoreType.DMA
    vmem = pltpu.VMEM
    gain = norm_gain[None, :]

    half = HEAD_DIM // 2
    freq = 10000.0 ** (-np.arange(half, dtype=np.float64) / half)
    freq = np.concatenate([freq, freq])
    sign = np.concatenate([-np.ones(half), np.ones(half)])
    a = np.arange(seq // LONG)[:, None] * float(LONG) * freq
    b = np.arange(SHORT)[:, None] * freq
    tc, ts = np.cos(a).astype(np.float32), (np.sin(a) * sign).astype(np.float32)
    bc, bs = np.cos(b).astype(np.float32), (np.sin(b) * sign).astype(np.float32)

    proj = 2.0 * rows * model * width
    other_tokens = swap(tokens)
    act = sds((rows, width), bf16)
    table = sds((rows, HEAD_DIM), f32)
    u_shape = sds((d.chunks, heads, HEAD_DIM, HEAD_DIM), f32)
    normed = sds((rows, model), bf16)
    weight = sds((model, width), bf16)
    scales = sds((heads, CHUNK, HEAD_DIM), f32)
    acc_scratch = vmem((rows, width), f32)
    (
        xn_own, k_own, v_own, u_own, cos_own, sin_own, cos_par, sin_par, wk, wv, gain_v, pos, neg,
    ) = call(
        functools.partial(own_keys, d),
        [
            normed, act, act, u_shape, table, table, table, table, weight, weight,
            sds((1, model), f32), scales, scales,
        ],
        "hhhhhhhh",
        [
            vmem((rows, model), bf16), vmem((2, n, HEAD_DIM), f32), vmem((2, n, HEAD_DIM), f32),
            vmem((SHORT, HEAD_DIM), f32), vmem((SHORT, HEAD_DIM), f32), acc_scratch,
            vmem((rows, width), bf16), dma((11,)),
        ],
        16, 2.4 * proj, (tokens, gain, tc, ts, bc, bs, w_key, w_value),
    )
    message = sds((width, HEAD_DIM), bf16)
    near, mirror = [(0, 1), (1, 0), (2, 3), (3, 2)], [(0, 3), (3, 0), (1, 2), (2, 1)]
    xn_par, k_par, v_par, u_par, state = call(
        functools.partial(partner_keys, d),
        [normed, act, act, u_shape, message],
        "vvvvvvvv", [acc_scratch, vmem((rows, width), bf16)],
        16, 2.4 * proj, (other_tokens, gain_v, cos_par, sin_par, wk, wv, neg, u_own),
    )
    got1 = lax.ppermute(state, "sp_1", near)
    pool_in, tail, wq, wop = call(
        functools.partial(pool_inputs, d),
        [sds((d.block, width), bf16), sds((RIM, width), bf16)],
        "vvv", [], 16, 2.2 * proj, (xn_own, xn_par, w_pool), loads=(w_query, w_out_pool),
    )
    part = sds((rows, width), f32)
    q_own, o_own, wor = call(
        functools.partial(queries, d), [act, part], "vvvvvvv", [acc_scratch], 16, 1.8 * proj,
        (xn_own, k_own, v_own, cos_own, sin_own, pos, wq), loads=(w_out_ret,),
    )
    pair = call(functools.partial(pair_states, d), message, "vv", [], 4, 0.1 * proj, (state, got1))
    got2 = lax.ppermute(pair, "sp_1", mirror)
    blocks = seq // d.block
    rim = lax.ppermute(tail, SP, [(i, (i + 1) % blocks) for i in range(blocks)])
    other_pool_w = swap(wop)
    q_par, o_par, wg = call(
        functools.partial(queries, d), [act, part], "vvvvvvv", [acc_scratch], 16, 1.8 * proj,
        (xn_par, k_par, v_par, cos_par, sin_par, pos, wq), loads=(w_gate,),
    )
    g_own = call(
        gates, act, "vvv", [],
        16, 1.1 * proj, (xn_own, ret_gain[None], wg),
    )
    row, prefix = call(
        functools.partial(row_states, d), [message, sds((width, HEAD_DIM), f32)],
        "vvv", [], 4, 0.1 * proj, (got1, pair, got2),
    )
    got3 = lax.ppermute(row, "sp_0", near)
    other_ret_w = swap(wor)
    g_par = call(
        gates, act, "vvv", [],
        16, 1.1 * proj, (xn_par, ret_gain[None], wg),
    )
    p_own, p_par = call(
        functools.partial(pools, d), [act, act], "vvvvv",
        [vmem((d.block + RIM, width), bf16), vmem((d.block, width), bf16), vmem((d.block, width), bf16)],
        16, 1.0 * proj, (pool_in, rim, pool_mix, pool_bias, pool_gain[None]),
    )
    p_recv = swap(p_par)
    column = call(
        functools.partial(column_states, d), message, "vv", [], 4, 0.1 * proj, (row, got3)
    )
    got4 = lax.ppermute(column, "sp_0", mirror)
    base_own, base_par = call(
        functools.partial(chunk_bases, d), [u_shape, u_shape], "vvvv", [],
        12, 0.2 * proj, (prefix, got3, u_own, u_par),
    )
    acc = call(
        pool_outputs, normed_f32(rows, model), "vvvv", [],
        12, 2.0 * proj, (p_own, p_recv, wop, other_pool_w),
    )
    s_scratch = vmem((d.chunks, heads // 2, 2 * HEAD_DIM, 2 * HEAD_DIM), bf16)
    ret_par = call(
        functools.partial(partner_retention, d),
        act, "vvvvv", [s_scratch], 12, 0.5 * proj,
        (q_par, o_par, g_par, base_par, got4),
    )
    ret_recv = swap(ret_par)
    acc = call(
        functools.partial(own_retention, d),
        normed_f32(rows, model), "vvvvvvv", [s_scratch, vmem((rows, width), bf16)],
        12, 1.5 * proj,
        (q_own, o_own, g_own, base_own, got4, acc, wor),
    )
    return call(
        last_share, normed, "vvv",
        [vmem((rows, model), bf16), dma((model // 512,))],
        12, 1.0 * proj, (acc, ret_recv, other_ret_w), outs_hbm=True,
    )


def solution(mesh):
    finer = Mesh(
        mesh.devices.reshape(4, 4, mesh.shape["fs"], mesh.shape["tp"]), ("sp_0", "sp_1", "fs", "tp")
    )
    placed = (
        P(FS_SP_TP, None), P(), P(None, "tp"), P(None, "tp"), P(None, "tp"), P(None, "tp"),
        P(None, "tp"), P("tp", None, None), P("tp", None), P("tp"), P("tp"), P("tp", None),
        P("tp", None),
    )

    def layer(seq, *args):
        return per_device(seq, *args)

    def whole(tokens, *rest):
        seq = tokens.shape[0] // mesh.shape["fs"]
        return jax.shard_map(
            functools.partial(layer, seq), mesh=finer, in_specs=placed,
            out_specs=P(FS_SP_TP, None), check_vma=False,
        )(tokens, *rest)

    return whole
```
